512 devices in a mesh: grp: 2 (over y), sp: 64 (over z, core), tp: 4 (over x).
Axes of the slice: x: 4, y: 2, z: 32, core: 2. Of those that a mesh axis runs over, the one named last changes fastest.
The devices are a block of a 4x8x32 slice.
Arguments:
- tokens: bfloat16 [32768, 4096], P(('grp', 'sp'), 'tp'), parts along dimension 0, may hold values from -45 to 45
- norm_gain: float32 [2, 4096], replicated, may hold values from 0.1 to 1.9
- value_weight: bfloat16 [2, 4096, 1024], P(None, 'sp', 'tp'), may hold values from -0.09375 to 0.09375
- gate_weight: bfloat16 [2, 4096, 1024], P(None, 'sp', 'tp'), may hold values from -0.09375 to 0.09375
- conv_taps: float32 [2, 31, 1024], P(None, None, 'tp'), may hold values from -4 to 4
- channel_gain: float32 [2, 1024], P(None, 'tp'), may hold values from 0.1 to 1.9
- out_weight: bfloat16 [2, 1024, 4096], P(None, 'sp', 'tp'), may hold values from -0.375 to 0.375
- final_gain: float32 [4096], P('tp'), may hold values from 0.1 to 1.9
Outputs:
- result: bfloat16 [32768, 4096], P(('grp', 'sp'), 'tp'), parts along dimension 0
The draws below stay inside these ranges and needn't reach their ends.
There are 2 independent parts, one for each index of `grp`. The reference program is written for one: setup_inputs(seed, part) draws one part's arguments, and reference() takes and returns one part's arrays. A program takes and returns all parts, laid end to end along the dimension named above; an argument that names none is the same for every part. Nothing has to cross between parts.
All inputs are finite; a program needn't handle non-finite values.
Results may differ from the reference program's by a relative error of at most 0.012.
Values may be sent and summed in bfloat16 or wider, within the bound.
No kernel may reach another device: no remote copies, remote signals or barrier semaphores. Data moves between devices by JAX's collectives and lax.ppermute only.
A program may use at most 128 MiB of HBM per device.

```python
import jax
import jax.numpy as jnp
from jax import lax

D = 4096
C = 1024
KERNEL = 31
LAYERS = 2
TOKENS = 16384


def draw_tokens(key, part):
    key_base, key_cols, key_rows = jax.random.split(key, 3)
    cols = jnp.arange(D, dtype=jnp.float32) / D
    col_scale = jnp.exp(jnp.log(3.0) * cols) * jnp.exp(jax.random.uniform(key_cols, (D,), jnp.float32, -0.35, 0.35))
    row_scale = jnp.exp(jax.random.uniform(key_rows, (TOKENS, 1), jnp.float32, -0.69, 0.69))
    base = jnp.clip(jax.random.normal(key_base, (TOKENS, D), jnp.float32), -4.0, 4.0)
    return (base * col_scale[None, :] * row_scale).astype(jnp.bfloat16)


def draw_conv_taps(key, part):
    key_base, key_cols = jax.random.split(key, 2)
    cols = jnp.arange(C, dtype=jnp.float32) / C
    col_scale = jnp.exp(jnp.log(3.0) * cols) * jnp.exp(jax.random.uniform(key_cols, (LAYERS, 1, C), jnp.float32, -0.5, 0.5))
    base = jnp.clip(jax.random.normal(key_base, (LAYERS, KERNEL, C), jnp.float32), -4.0, 4.0)
    return base * col_scale * KERNEL ** (-0.5)


def levels(key, shape, cuts, low, top_value):
    factor_of, own = 1.0, jax.random.fold_in(key, 6)
    for position, parts in cuts:
        steps = jnp.exp(jax.random.uniform(jax.random.fold_in(own, position), (parts,), jnp.float32, low / len(cuts), top_value / len(cuts)))
        factor_of = factor_of * jnp.repeat(steps, shape[position] // parts).reshape([-1 if axis == position else 1 for axis in range(len(shape))])
    return factor_of


def noise(own_key, dims, scale, most, pieces=(), held_as=jnp.bfloat16):
    entries = scale * jax.random.normal(own_key, dims, jnp.float32)
    if pieces:
        entries = entries * levels(own_key, dims, pieces, -0.22, 0.18)
    return jnp.clip(entries, -most, most).astype(held_as)


def setup_inputs(seed: int = 0, part: int = 0) -> dict:
    keys = jax.random.split(jax.random.key(seed), 9)
    part_keys = jax.random.split(jax.random.fold_in(keys[8], part), 9)
    return {
        "tokens": draw_tokens(jax.random.fold_in(jax.random.fold_in(keys[8], part), 71), part),
        "norm_gain": jnp.clip(1.0 + 0.18 * jax.random.normal(keys[1], (LAYERS, D), jnp.float32), 0.1, 1.9),
        "value_weight": noise(keys[2], (LAYERS, D, C), D ** -0.5, 0.09375, ((1, 64), (2, 4))),
        "gate_weight": noise(keys[3], (LAYERS, D, C), D ** -0.5, 0.09375, ((1, 64), (2, 4))),
        "conv_taps": draw_conv_taps(jax.random.fold_in(keys[8], 71), part),
        "channel_gain": jnp.clip(1.0 + 0.18 * jax.random.normal(keys[5], (LAYERS, C), jnp.float32), 0.1, 1.9),
        "out_weight": noise(keys[6], (LAYERS, C, D), (C // 4) ** -0.5, 0.375, ((1, 64), (2, 4))),
        "final_gain": jnp.clip(1.0 + 0.18 * jax.random.normal(keys[7], (D,), jnp.float32), 0.1, 1.9),
    }


def depthwise(glu, taps):
    reach = taps.shape[0] // 2
    padded = jnp.pad(glu.astype(jnp.float32), ((reach, reach), (0, 0)))
    length = glu.shape[0]
    total = jnp.zeros(glu.shape, jnp.float32)
    for tap in range(taps.shape[0]):
        total = total + taps[tap][None, :] * padded[tap:tap + length]
    return total

def reference(tokens, norm_gain, value_weight, gate_weight, conv_taps, channel_gain, out_weight, final_gain):
    x_state = tokens
    for layer in range(LAYERS):
        xf = x_state.astype(jnp.float32)
        scale = lax.rsqrt(lax.optimization_barrier(jnp.mean(xf * xf, axis=1, keepdims=True)) + 1e-06)
        normed = (xf * scale * norm_gain[layer][None, :]).astype(jnp.bfloat16)
        value = jnp.dot(normed, value_weight[layer], preferred_element_type=jnp.float32)
        gate = jnp.dot(normed, gate_weight[layer], preferred_element_type=jnp.float32)
        glu = (value * jax.nn.sigmoid(gate)).astype(jnp.bfloat16)
        conv = depthwise(glu, conv_taps[layer])
        center = lax.optimization_barrier(jnp.mean(conv, axis=1, keepdims=True))
        shifted = conv - center
        spread = lax.optimization_barrier(jnp.mean(shifted * shifted, axis=1, keepdims=True))
        act = jax.nn.silu(shifted * lax.rsqrt(spread + 1e-05) * channel_gain[layer][None, :]).astype(jnp.bfloat16)
        branch = jnp.dot(act, out_weight[layer], preferred_element_type=jnp.float32)
        x_state = (xf + branch).astype(jnp.bfloat16)
    xf = x_state.astype(jnp.float32)
    scale = lax.rsqrt(lax.optimization_barrier(jnp.mean(xf * xf, axis=1, keepdims=True)) + 1e-06)
    return (xf * scale * final_gain[None, :]).astype(jnp.bfloat16)
```

```python
import jax
import jax.numpy as jnp
from jax import lax
from jax.sharding import PartitionSpec as P

LAYERS = 2
IN_SCALE = 2.0**19
OUT_SCALE = 2.0**17
X_SCALE = 2.0**6


def exchanged(value, axis):
    size = lax.axis_size(axis)
    return lax.all_to_all(
        jnp.broadcast_to(value[None], (size, *value.shape)), axis, 0, 0, tiled=True
    )


def joined(pieces):
    size, rows, width = pieces.shape
    return jnp.moveaxis(pieces, 0, 1).reshape(rows, size * width)


def with_neighbours(block, axis, width):
    count = lax.axis_size(axis)
    forward = [(i, i + 1) for i in range(count - 1)]
    backward = [(i + 1, i) for i in range(count - 1)]
    low = lax.ppermute(block[block.shape[0] - width :], axis, forward)
    high = lax.ppermute(block[:width], axis, backward)
    return jnp.concatenate([low, block, high], axis=0)


def packed(value, gate, out):
    width = value.shape[1] + gate.shape[1]
    projections = jnp.concatenate([value, gate], axis=1).astype(jnp.float32) * IN_SCALE
    out = out.astype(jnp.float32) * OUT_SCALE
    halves = [out[:, i : i + width] for i in range(0, out.shape[1], width)]
    return [projections.astype(jnp.float16)] + [h.astype(jnp.float16) for h in halves]


def unpacked(gathered, rows):
    parts, _, width = gathered.shape
    return gathered[:, rows].astype(jnp.bfloat16).reshape(-1, width)


def split_in_three(value):
    parts = []
    for _ in range(3):
        part = lax.reduce_precision(value, 8, 7)
        parts.append(part.astype(jnp.bfloat16))
        value = value - part
    return parts


def convolved(xf, projections, gain, taps, rows):
    scale = lax.rsqrt(jnp.mean(xf * xf, axis=1, keepdims=True) + 1e-06)
    normed = (xf * scale * gain[None, :]).astype(jnp.bfloat16)
    both = jnp.dot(normed, projections, preferred_element_type=jnp.float32) * (1 / IN_SCALE)
    half = both.shape[1] // 2
    value, gate = both[:, :half], both[:, half:]
    glu = (value * jax.nn.sigmoid(gate)).astype(jnp.bfloat16).astype(jnp.float32)
    reach = taps.shape[0] // 2
    first = (glu.shape[0] - rows) // 2 - reach
    conv = jnp.zeros((rows, half), jnp.float32)
    for tap in range(taps.shape[0]):
        conv = conv + taps[tap][None, :] * glu[first + tap : first + tap + rows]
    return conv.astype(jnp.bfloat16)


def projected(conv, gain, outs):
    conv = conv.astype(jnp.float32)
    center = jnp.mean(conv, axis=1, keepdims=True)
    shifted = conv - center
    spread = jnp.mean(shifted * shifted, axis=1, keepdims=True)
    act = jax.nn.silu(shifted * lax.rsqrt(spread + 1e-05) * gain[None, :]).astype(jnp.bfloat16)
    branch = [jnp.dot(act, o, preferred_element_type=jnp.float32) * (1 / OUT_SCALE) for o in outs]
    return jnp.concatenate(branch, axis=1)


def on_device(
    tokens, norm_gain, value_weight, gate_weight, conv_taps, channel_gain, out_weight, final_gain
):
    rows = tokens.shape[0]
    margin = 16
    x_local = with_neighbours(tokens, "sp", 2 * margin)
    coded = jnp.stack(split_in_three(channel_gain)).reshape(-1)
    width = tokens.shape[1]
    coded = jnp.pad(coded, (0, 2 * width - coded.shape[0])).reshape(2, width)
    sent = jnp.concatenate([coded[:1], x_local[1:-1], coded[1:]], axis=0)
    everyone = exchanged(sent, "tp")
    x_all = joined(everyone)
    gains = jnp.concatenate([everyone[:, 0], everyone[:, -1]], axis=1)[:, : 3 * channel_gain.size]
    gains = gains.reshape(-1, 3, *channel_gain.shape).astype(jnp.float32)
    gains = gains[:, 0] + (gains[:, 1] + gains[:, 2])
    gains = jnp.moveaxis(gains, 0, 1).reshape(LAYERS, -1)
    pieces = []
    for l in range(LAYERS):
        pieces += packed(value_weight[l], gate_weight[l], out_weight[l])
    weights = lax.all_gather(jnp.concatenate(pieces, axis=0), "sp")
    starts, at = [], 0
    for piece in pieces:
        starts.append(slice(at, at + piece.shape[0]))
        at += piece.shape[0]
    per = len(pieces) // LAYERS

    middle = rows + 2 * margin
    projections = unpacked(weights, starts[0])
    conv = convolved(
        x_all.astype(jnp.float32), projections, norm_gain[0], conv_taps[0], middle
    )
    conv, weights = lax.optimization_barrier((conv, weights))
    conv_all = joined(exchanged(conv, "tp"))
    outs = [unpacked(weights, s) for s in starts[1:per]]
    projections = unpacked(weights, starts[per])
    branch = projected(conv_all, gains[0], outs)
    position = lax.axis_index("sp") * rows - margin + lax.iota(jnp.int32, middle)
    inside = (position >= 0) & (position < rows * lax.axis_size("sp"))
    x_next = x_local[margin : margin + middle].astype(jnp.float32) + branch
    x_next = jnp.where(inside[:, None], x_next, 0.0).astype(jnp.bfloat16)

    shared = (x_next.astype(jnp.float32) * X_SCALE).astype(jnp.float16)
    x_all = joined(lax.all_gather(shared, "tp")).astype(jnp.float32) * (1 / X_SCALE)
    conv = convolved(x_all, projections, norm_gain[1], conv_taps[1], rows)
    conv, weights = lax.optimization_barrier((conv, weights))
    conv_all = joined(exchanged(conv, "tp"))
    outs = [unpacked(weights, s) for s in starts[per + 1 :]]
    branch = projected(conv_all, gains[1], outs)
    x_last = (x_next[margin : margin + rows].astype(jnp.float32) + branch).astype(jnp.bfloat16)

    xf = x_last.astype(jnp.float32)
    squares = jnp.sum(exchanged(jnp.sum(xf * xf, axis=1), "tp"), axis=0)
    width = xf.shape[1] * lax.axis_size("tp")
    scale = lax.rsqrt(squares / width + 1e-06)[:, None]
    return (xf * scale * final_gain[None, :]).astype(jnp.bfloat16)


def solution(mesh):
    placed = (
        P(("grp", "sp"), "tp"),
        P(),
        P(None, "sp", "tp"),
        P(None, "sp", "tp"),
        P(None, None, "tp"),
        P(None, "tp"),
        P(None, "sp", "tp"),
        P("tp"),
    )
    return jax.shard_map(
        on_device, mesh=mesh, in_specs=placed, out_specs=P(("grp", "sp"), "tp"), check_vma=False
    )
```

```python
import functools

import jax
import jax.numpy as jnp
from jax import lax
from jax.experimental import pallas as pl
from jax.experimental.pallas import tpu as pltpu
from jax.sharding import PartitionSpec as P

LAYERS = 2
IN_SCALE = 2.0**19
OUT_SCALE = 2.0**17
X_SCALE = 2.0**6


def exchanged(value, axis):
    size = lax.axis_size(axis)
    return lax.all_to_all(
        jnp.broadcast_to(value[None], (size, *value.shape)), axis, 0, 0, tiled=True
    )


def joined(pieces):
    size, rows, width = pieces.shape
    return jnp.moveaxis(pieces, 0, 1).reshape(rows, size * width)


def neighbours(block, axis, width):
    count = lax.axis_size(axis)
    forward = [(i, i + 1) for i in range(count - 1)]
    backward = [(i + 1, i) for i in range(count - 1)]
    low = lax.ppermute(block[block.shape[0] - width :], axis, forward)
    high = lax.ppermute(block[:width], axis, backward)
    return low, high


def packed(value, gate, out):
    width = value.shape[1] + gate.shape[1]
    projections = jnp.concatenate([value, gate], axis=1).astype(jnp.float32) * IN_SCALE
    out = out.astype(jnp.float32) * OUT_SCALE
    halves = [out[:, i : i + width] for i in range(0, out.shape[1], width)]
    return [projections.astype(jnp.float16)] + [h.astype(jnp.float16) for h in halves]


def unpacked(gathered, rows):
    parts, _, width = gathered.shape
    return gathered[:, rows].astype(jnp.bfloat16).reshape(-1, width)


def split_in_three(value):
    parts = []
    for _ in range(3):
        part = lax.reduce_precision(value, 8, 7)
        parts.append(part.astype(jnp.bfloat16))
        value = value - part
    return parts


def convolved_kernel(first, x_ref, w_ref, gain_ref, taps_ref, out_ref, scaled_ref, glu_ref):
    pieces, rows_in, width = x_ref.shape
    count, rows, half = out_ref.shape
    block = 32
    blocks = range(0, rows_in, block)

    squares = [jnp.zeros((block, 128), jnp.float32) for _ in blocks]
    both = None
    for j in range(pieces):
        for i, at in enumerate(blocks):
            for b in range(0, width, 128):
                xf = x_ref[j, at : at + block, b : b + 128].astype(jnp.float32)
                squares[i] = squares[i] + xf * xf
                scaled = (xf * gain_ref[j, :, b : b + 128]).astype(jnp.bfloat16)
                scaled_ref[j, at : at + block, b : b + 128] = scaled
        part = jnp.dot(scaled_ref[j], w_ref[j], preferred_element_type=jnp.float32)
        both = part if both is None else both + part
    for i, at in enumerate(blocks):
        mean = jnp.sum(squares[i], axis=1, keepdims=True) / (pieces * width)
        scale = lax.rsqrt(mean + 1e-06) * (1 / IN_SCALE)
        value = both[at : at + block, :half] * scale
        gate = both[at : at + block, half:] * scale
        glu = (value * jax.nn.sigmoid(gate)).astype(jnp.bfloat16)
        glu_ref[0, at : at + block, :] = glu.astype(jnp.float32)
    reach_rows = rows_in - 8
    for shift in range(1, 8):
        glu_ref[shift, :reach_rows, :] = glu_ref[0, shift : shift + reach_rows, :]

    def convolve(i, carry):
        base = pl.multiple_of(i * block, block)
        for lane in range(0, half, 128):
            lanes = slice(lane, lane + 128)
            conv = jnp.zeros((block, 128), jnp.float32)
            for tap in range(taps_ref.shape[0]):
                down, shift = divmod(first + tap, 8)
                moved = glu_ref[shift, pl.ds(pl.multiple_of(base + 8 * down, 8), block), lanes]
                conv = conv + taps_ref[tap : tap + 1, lanes] * moved
            conv = conv.astype(jnp.bfloat16)
            for c in range(count):
                out_ref[c, pl.ds(base, block), lanes] = conv
        return carry

    lax.fori_loop(0, rows // block, convolve, 0)


def convolved(pieces, projections, gain, taps, rows):
    count, rows_in, width = pieces.shape
    both = projections.shape[1]
    half = both // 2
    first = (rows_in - rows) // 2 - taps.shape[0] // 2
    vmem = pl.BlockSpec(memory_space=pltpu.VMEM)
    return pl.pallas_call(
        functools.partial(convolved_kernel, first),
        out_shape=jax.ShapeDtypeStruct((count, rows, half), jnp.bfloat16),
        in_specs=[vmem] * 4,
        out_specs=vmem,
        scratch_shapes=[
            pltpu.VMEM((count, rows_in, width), jnp.bfloat16),
            pltpu.VMEM((8, rows_in, half), jnp.float32),
        ],
        cost_estimate=pl.CostEstimate(
            flops=2 * rows_in * count * width * both,
            bytes_accessed=2 * (count * width * both + count * rows_in * width),
            transcendentals=rows_in * half,
        ),
    )(
        pieces,
        projections.reshape(count, width, both),
        gain.reshape(count, 1, width),
        taps,
    )


def projected(conv, gain, outs):
    conv = conv.astype(jnp.float32)
    center = jnp.mean(conv, axis=1, keepdims=True)
    shifted = conv - center
    spread = jnp.mean(shifted * shifted, axis=1, keepdims=True)
    act = jax.nn.silu(shifted * lax.rsqrt(spread + 1e-05) * gain[None, :]).astype(jnp.bfloat16)
    branch = [jnp.dot(act, o, preferred_element_type=jnp.float32) * (1 / OUT_SCALE) for o in outs]
    return jnp.concatenate(branch, axis=1)


def on_device(
    tokens, norm_gain, value_weight, gate_weight, conv_taps, channel_gain, out_weight, final_gain
):
    rows = tokens.shape[0]
    margin = 16
    low, high = neighbours(tokens, "sp", 2 * margin)
    coded = jnp.stack(split_in_three(channel_gain)).reshape(-1)
    width = tokens.shape[1]
    coded = jnp.pad(coded, (0, 2 * width - coded.shape[0])).reshape(2, width)
    x_local = jnp.concatenate([low, tokens, high], axis=0)
    everyone = exchanged(jnp.concatenate([coded[:1], x_local[1:-1], coded[1:]], axis=0), "tp")
    x_local = x_local[margin:-margin]
    gains = jnp.concatenate([everyone[:, 0], everyone[:, -1]], axis=1)[:, : 3 * channel_gain.size]
    gains = gains.reshape(-1, 3, *channel_gain.shape).astype(jnp.float32)
    gains = gains[:, 0] + (gains[:, 1] + gains[:, 2])
    gains = jnp.moveaxis(gains, 0, 1).reshape(LAYERS, -1)
    pieces = []
    for l in range(LAYERS):
        pieces += packed(value_weight[l], gate_weight[l], out_weight[l])
    weights = lax.all_gather(jnp.concatenate(pieces, axis=0), "sp")
    starts, at = [], 0
    for piece in pieces:
        starts.append(slice(at, at + piece.shape[0]))
        at += piece.shape[0]
    per = len(pieces) // LAYERS

    middle = rows + 2 * margin
    projections = unpacked(weights, starts[0])
    conv = convolved(everyone, projections, norm_gain[0], conv_taps[0], middle)
    conv, weights = lax.optimization_barrier((conv, weights))
    conv_all = joined(lax.all_to_all(conv, "tp", 0, 0, tiled=True))
    outs = [unpacked(weights, s) for s in starts[1:per]]
    projections = unpacked(weights, starts[per])
    branch = projected(conv_all, gains[0], outs)
    position = lax.axis_index("sp") * rows - margin + lax.iota(jnp.int32, middle)
    inside = (position >= 0) & (position < rows * lax.axis_size("sp"))
    x_next = x_local.astype(jnp.float32) + branch
    x_next = jnp.where(inside[:, None], x_next, 0.0).astype(jnp.bfloat16)

    shared = (x_next.astype(jnp.float32) * X_SCALE).astype(jnp.float16)
    x_all = lax.all_gather(shared, "tp").astype(jnp.float32) * (1 / X_SCALE)
    conv = convolved(x_all.astype(jnp.bfloat16), projections, norm_gain[1], conv_taps[1], rows)
    conv, weights = lax.optimization_barrier((conv, weights))
    conv_all = joined(lax.all_to_all(conv, "tp", 0, 0, tiled=True))
    outs = [unpacked(weights, s) for s in starts[per + 1 :]]
    branch = projected(conv_all, gains[1], outs)
    x_last = (x_next[margin : margin + rows].astype(jnp.float32) + branch).astype(jnp.bfloat16)

    xf = x_last.astype(jnp.float32)
    squares = jnp.sum(exchanged(jnp.sum(xf * xf, axis=1), "tp"), axis=0)
    width = xf.shape[1] * lax.axis_size("tp")
    scale = lax.rsqrt(squares / width + 1e-06)[:, None]
    return (xf * scale * final_gain[None, :]).astype(jnp.bfloat16)


def solution(mesh):
    placed = (
        P(("grp", "sp"), "tp"),
        P(),
        P(None, "sp", "tp"),
        P(None, "sp", "tp"),
        P(None, None, "tp"),
        P(None, "tp"),
        P(None, "sp", "tp"),
        P("tp"),
    )
    return jax.shard_map(
        on_device, mesh=mesh, in_specs=placed, out_specs=P(("grp", "sp"), "tp"), check_vma=False
    )
```

```python
import functools

import jax
import jax.numpy as jnp
from jax import lax
from jax.experimental import pallas as pl
from jax.experimental.pallas import tpu as pltpu
from jax.sharding import PartitionSpec as P

LAYERS = 2
IN_SCALE = 2.0**19
OUT_SCALE = 2.0**17
X_SCALE = 2.0**6


def exchanged(value, axis):
    size = lax.axis_size(axis)
    return lax.all_to_all(
        jnp.broadcast_to(value[None], (size, *value.shape)), axis, 0, 0, tiled=True
    )


def joined(pieces):
    size, rows, width = pieces.shape
    return jnp.moveaxis(pieces, 0, 1).reshape(rows, size * width)


def neighbours(block, axis, width):
    count = lax.axis_size(axis)
    forward = [(i, i + 1) for i in range(count - 1)]
    backward = [(i + 1, i) for i in range(count - 1)]
    low = lax.ppermute(block[block.shape[0] - width :], axis, forward)
    high = lax.ppermute(block[:width], axis, backward)
    return low, high


def packed_kernel(paired, order_ref, value_ref, gate_ref, out_ref, sent_ref):
    rows, channels = value_ref.shape[1:]
    out_rows, features = out_ref.shape[1:]
    half = channels // 2
    upper = order_ref[0] != 0
    at = 0

    def projection(layer, lower):
        lanes = slice(0, half) if lower else slice(half, channels)
        pair = value_ref[layer, :, lanes], gate_ref[layer, :, lanes]
        return [p.astype(jnp.float32) * IN_SCALE for p in pair]

    for layer in range(LAYERS):
        blocks = [projection(layer, True), projection(layer, False)]
        if paired and layer == LAYERS - 1:
            blocks = [[jnp.where(upper, high, low) for low, high in zip(*blocks)]]
        for value, gate in blocks:
            sent_ref[at : at + rows, :half] = value.astype(jnp.bfloat16)
            sent_ref[at : at + rows, half:] = gate.astype(jnp.bfloat16)
            at += rows
        for i in range(0, features, channels):
            block = out_ref[layer, :, i : i + channels].astype(jnp.float32) * OUT_SCALE
            sent_ref[at : at + out_rows] = block.astype(jnp.bfloat16)
            at += out_rows


def packed(value, gate, out, order, paired):
    rows, channels = value.shape[1:]
    out_rows, features = out.shape[1:]
    slices, at = [], 0
    for layer in range(LAYERS):
        of_layer = []
        for _ in range(1 if paired and layer == LAYERS - 1 else 2):
            of_layer.append(slice(at, at + rows))
            at += rows
        of_layer.append(slice(at, at + out_rows * (features // channels)))
        at = of_layer[-1].stop
        slices.append(of_layer)
    vmem = pl.BlockSpec(memory_space=pltpu.VMEM)
    sent = pl.pallas_call(
        functools.partial(packed_kernel, paired),
        out_shape=jax.ShapeDtypeStruct((at, channels), jnp.bfloat16),
        in_specs=[pl.BlockSpec(memory_space=pltpu.SMEM), vmem, vmem, vmem],
        out_specs=vmem,
    )(order.reshape(1), value, gate, out)
    return sent, slices


def out_product(act, block, rows):
    parts, height, width = block.shape
    return jnp.concatenate(
        [
            jnp.dot(
                act,
                block[:, i : i + rows].reshape(parts * rows, width),
                preferred_element_type=jnp.float32,
            )
            for i in range(0, height, rows)
        ],
        axis=1,
    ) * (1 / OUT_SCALE)


def split_in_three(value):
    parts = []
    for _ in range(3):
        part = lax.reduce_precision(value, 8, 7)
        parts.append(part.astype(jnp.bfloat16))
        value = value - part
    return parts


def convolved_kernel(
    first, order_ref, x_ref, a_ref, b_ref, gain_ref, taps_ref, out_ref,
    scaled_ref, squares_ref, total_ref, glu_ref,
):
    step = pl.program_id(0)
    _, rows_in, width = x_ref.shape
    count, rows, channels = out_ref.shape
    half = channels // 2
    block = 32
    blocks = range(0, rows_in, block)

    @pl.when(step == 0)
    def _():
        squares_ref[...] = jnp.zeros_like(squares_ref)
        total_ref[...] = jnp.zeros_like(total_ref)

    for at in blocks:
        square = squares_ref[at : at + block]
        for b in range(0, width, 128):
            xf = x_ref[0, at : at + block, b : b + 128].astype(jnp.float32)
            square = square + xf * xf
            scaled = (xf * gain_ref[0, :, b : b + 128]).astype(jnp.bfloat16)
            scaled_ref[at : at + block, b : b + 128] = scaled
        squares_ref[at : at + block] = square
    for k, w_ref in enumerate((a_ref, b_ref)):
        total_ref[k] += jnp.dot(scaled_ref[...], w_ref[0], preferred_element_type=jnp.float32)

    @pl.when(step == pl.num_programs(0) - 1)
    def _():
        swapped = order_ref[0] != 0
        for at in blocks:
            mean = jnp.sum(squares_ref[at : at + block], axis=1, keepdims=True)
            mean = mean / (pl.num_programs(0) * width)
            scale = lax.rsqrt(mean + 1e-06) * (1 / IN_SCALE)
            glu = []
            for k in range(2):
                value = total_ref[k, at : at + block, :half] * scale
                gate = total_ref[k, at : at + block, half:] * scale
                gated = (value * jax.nn.sigmoid(gate)).astype(jnp.bfloat16)
                glu.append(gated.astype(jnp.float32))
            glu_ref[0, at : at + block, :half] = jnp.where(swapped, glu[1], glu[0])
            glu_ref[0, at : at + block, half:] = jnp.where(swapped, glu[0], glu[1])
        reach_rows = rows_in - 8
        for shift in range(1, 8):
            glu_ref[shift, :reach_rows, :] = glu_ref[0, shift : shift + reach_rows, :]

        def convolve(i, carry):
            base = pl.multiple_of(i * block, block)
            for lane in range(0, channels, 128):
                lanes = slice(lane, lane + 128)
                conv = jnp.zeros((block, 128), jnp.float32)
                for tap in range(taps_ref.shape[0]):
                    down, shift = divmod(first + tap, 8)
                    moved = glu_ref[shift, pl.ds(pl.multiple_of(base + 8 * down, 8), block), lanes]
                    conv = conv + taps_ref[tap : tap + 1, lanes] * moved
                conv = conv.astype(jnp.bfloat16)
                for c in range(count):
                    out_ref[c, pl.ds(base, block), lanes] = conv
            return carry

        lax.fori_loop(0, rows // block, convolve, 0)


def convolved(pieces, blocks, order, gain, taps, rows):
    count, rows_in, width = pieces.shape
    channels = taps.shape[1]
    first = (rows_in - rows) // 2 - taps.shape[0] // 2
    blocks = [b.reshape(count, width, channels) for b in blocks]
    along = lambda *shape: pl.BlockSpec((1, *shape), lambda j: (j, 0, 0))
    return pl.pallas_call(
        functools.partial(convolved_kernel, first),
        grid=(count,),
        out_shape=jax.ShapeDtypeStruct((count, rows, channels), jnp.bfloat16),
        in_specs=[
            pl.BlockSpec(memory_space=pltpu.SMEM),
            along(rows_in, width),
            along(width, channels),
            along(width, channels),
            along(1, width),
            pl.BlockSpec(taps.shape, lambda j: (0, 0)),
        ],
        out_specs=pl.BlockSpec((count, rows, channels), lambda j: (0, 0, 0)),
        scratch_shapes=[
            pltpu.VMEM((rows_in, width), jnp.bfloat16),
            pltpu.VMEM((rows_in, 128), jnp.float32),
            pltpu.VMEM((2, rows_in, channels), jnp.float32),
            pltpu.VMEM((8, rows_in, channels), jnp.float32),
        ],
        cost_estimate=pl.CostEstimate(
            flops=4 * rows_in * count * width * channels,
            bytes_accessed=4 * count * width * channels + 2 * count * rows_in * width,
            transcendentals=rows_in * channels,
        ),
    )(order.reshape(1), pieces, *blocks, gain.reshape(count, 1, width), taps)


def activated(conv, gain):
    conv = conv.astype(jnp.float32)
    center = jnp.mean(conv, axis=1, keepdims=True)
    shifted = conv - center
    spread = jnp.mean(shifted * shifted, axis=1, keepdims=True)
    return jax.nn.silu(shifted * lax.rsqrt(spread + 1e-05) * gain[None, :]).astype(jnp.bfloat16)


def on_device(
    tokens, norm_gain, value_weight, gate_weight, conv_taps, channel_gain, out_weight, final_gain
):
    rows = tokens.shape[0]
    margin = 16
    low, high = neighbours(tokens, "sp", 2 * margin)
    coded = jnp.stack(split_in_three(channel_gain)).reshape(-1)
    width = tokens.shape[1]
    coded = jnp.pad(coded, (0, 2 * width - coded.shape[0])).reshape(2, width)
    x_local = jnp.concatenate([low, tokens, high], axis=0)
    everyone = exchanged(jnp.concatenate([coded[:1], x_local[1:-1], coded[1:]], axis=0), "tp")
    x_local = x_local[margin:-margin]
    gains = jnp.concatenate([everyone[:, 0], everyone[:, -1]], axis=1)[:, : 3 * channel_gain.size]
    gains = gains.reshape(-1, 3, *channel_gain.shape).astype(jnp.float32)
    gains = gains[:, 0] + (gains[:, 1] + gains[:, 2])
    gains = jnp.moveaxis(gains, 0, 1).reshape(LAYERS, -1)
    groups = lax.axis_size("grp")
    paired = groups % 2 == 0
    order = lax.axis_index("grp") % 2 if paired else jnp.int32(0)
    swap = [(i, i ^ 1) for i in range(groups)]
    out_rows = out_weight.shape[1]
    sent, slices = packed(value_weight, gate_weight, out_weight, order, paired)
    weights = lax.all_gather(sent.astype(jnp.float16), "sp")

    def taken(at):
        return weights[:, at].astype(jnp.bfloat16)

    late_blocks = [taken(at) for at in slices[1][:-1]]
    if paired:
        late_blocks.append(lax.ppermute(late_blocks[0], "grp", swap))
    middle = rows + 2 * margin
    conv = convolved(
        everyone, [taken(at) for at in slices[0][:-1]], jnp.int32(0), norm_gain[0], conv_taps[0], middle
    )
    conv, weights = lax.optimization_barrier((conv, weights))
    conv_all = joined(lax.all_to_all(conv, "tp", 0, 0, tiled=True))
    act = activated(conv_all, gains[0])
    branch = out_product(act, taken(slices[0][-1]), out_rows)
    position = lax.axis_index("sp") * rows - margin + lax.iota(jnp.int32, middle)
    inside = (position >= 0) & (position < rows * lax.axis_size("sp"))
    x_next = x_local.astype(jnp.float32) + branch
    x_next = jnp.where(inside[:, None], x_next, 0.0).astype(jnp.bfloat16)

    shared = (x_next.astype(jnp.float32) * X_SCALE).astype(jnp.float16)
    x_all = lax.all_gather(shared, "tp").astype(jnp.float32) * (1 / X_SCALE)
    conv = convolved(
        x_all.astype(jnp.bfloat16), late_blocks, order, norm_gain[1], conv_taps[1], rows
    )
    conv, weights = lax.optimization_barrier((conv, weights))
    conv_all = joined(lax.all_to_all(conv, "tp", 0, 0, tiled=True))
    act = activated(conv_all, gains[1])
    branch = out_product(act, taken(slices[1][-1]), out_rows)
    x_last = (x_next[margin : margin + rows].astype(jnp.float32) + branch).astype(jnp.bfloat16)

    xf = x_last.astype(jnp.float32)
    squares = jnp.sum(exchanged(jnp.sum(xf * xf, axis=1), "tp"), axis=0)
    width = xf.shape[1] * lax.axis_size("tp")
    scale = lax.rsqrt(squares / width + 1e-06)[:, None]
    return (xf * scale * final_gain[None, :]).astype(jnp.bfloat16)


def solution(mesh):
    placed = (
        P(("grp", "sp"), "tp"),
        P(),
        P(None, "sp", "tp"),
        P(None, "sp", "tp"),
        P(None, None, "tp"),
        P(None, "tp"),
        P(None, "sp", "tp"),
        P("tp"),
    )
    return jax.shard_map(
        on_device, mesh=mesh, in_specs=placed, out_specs=P(("grp", "sp"), "tp"), check_vma=False
    )
```

```python
import functools

import jax
import jax.numpy as jnp
from jax import lax
from jax.experimental import pallas as pl
from jax.experimental.pallas import tpu as pltpu
from jax.sharding import PartitionSpec as P


LAYERS = 2
IN_SCALE = 2.0**19
OUT_SCALE = 2.0**17
X_SCALE = 2.0**6


def exchanged(value, axis):
    size = lax.axis_size(axis)
    return lax.all_to_all(
        jnp.broadcast_to(value[None], (size, *value.shape)), axis, 0, 0, tiled=True
    )


def joined(pieces):
    size, rows, width = pieces.shape
    return jnp.moveaxis(pieces, 0, 1).reshape(rows, size * width)


def neighbours(block, axis, width):
    count = lax.axis_size(axis)
    forward = [(i, i + 1) for i in range(count - 1)]
    backward = [(i + 1, i) for i in range(count - 1)]
    low = lax.ppermute(block[block.shape[0] - width :], axis, forward)
    high = lax.ppermute(block[:width], axis, backward)
    return low, high


def packed_kernel(paired, order_ref, value_ref, gate_ref, out_ref, chan_ref, sent_ref, coded_ref):
    rows, channels = value_ref.shape[1:]
    out_rows, features = out_ref.shape[1:]
    half = channels // 2
    upper = order_ref[0] != 0
    at = 0

    def projection(layer, lower):
        lanes = slice(0, half) if lower else slice(half, channels)
        pair = value_ref[layer, :, lanes], gate_ref[layer, :, lanes]
        return [p.astype(jnp.float32) * IN_SCALE for p in pair]

    for layer in range(LAYERS):
        blocks = [projection(layer, True), projection(layer, False)]
        if paired and layer == LAYERS - 1:
            blocks = [[jnp.where(upper, high, low) for low, high in zip(*blocks)]]
        for value, gate in blocks:
            sent_ref[at : at + rows, :half] = value.astype(jnp.bfloat16)
            sent_ref[at : at + rows, half:] = gate.astype(jnp.bfloat16)
            at += rows
        starts = range(0, features, channels)
        blocks = [out_ref[layer, :, i : i + channels].astype(jnp.float32) * OUT_SCALE for i in starts]
        if paired and layer == LAYERS - 1:
            middle = len(blocks) // 2
            blocks = [jnp.where(upper, h, l) for l, h in zip(blocks[:middle], blocks[middle:])]
        for block in blocks:
            sent_ref[at : at + out_rows] = block.astype(jnp.bfloat16)
            at += out_rows
    coded_ref[...] = jnp.zeros_like(coded_ref)
    for layer in range(LAYERS):
        rest = chan_ref[layer : layer + 1, :]
        for part in range(3):
            row, lane = divmod((layer * 3 + part) * channels, coded_ref.shape[1])
            coded = rest.astype(jnp.bfloat16)
            coded_ref[row : row + 1, lane : lane + channels] = coded
            rest = rest - coded.astype(jnp.float32)


def packed(value, gate, out, chan_gain, order, paired):
    rows, channels = value.shape[1:]
    out_rows, features = out.shape[1:]
    slices, at = [], 0
    for layer in range(LAYERS):
        of_layer = []
        for _ in range(1 if paired and layer == LAYERS - 1 else 2):
            of_layer.append(slice(at, at + rows))
            at += rows
        share = 2 if paired and layer == LAYERS - 1 else 1
        of_layer.append(slice(at, at + out_rows * (features // channels) // share))
        at = of_layer[-1].stop
        slices.append(of_layer)
    vmem = pl.BlockSpec(memory_space=pltpu.VMEM)
    sent, coded = pl.pallas_call(
        functools.partial(packed_kernel, paired),
        out_shape=(
            jax.ShapeDtypeStruct((at, channels), jnp.bfloat16),
            jax.ShapeDtypeStruct((2, features), jnp.bfloat16),
        ),
        in_specs=[pl.BlockSpec(memory_space=pltpu.SMEM), vmem, vmem, vmem, vmem],
        out_specs=(vmem, vmem),
    )(order.reshape(1), value, gate, out, chan_gain)
    return sent, coded, slices


def out_product(act, block, rows):
    parts, height, width = block.shape
    return jnp.concatenate(
        [
            jnp.dot(
                act,
                block[:, i : i + rows].reshape(parts * rows, width),
                preferred_element_type=jnp.float32,
            )
            for i in range(0, height, rows)
        ],
        axis=1,
    ) * (1 / OUT_SCALE)


def convolved_kernel(
    first, layer, order_ref, x_ref, a_ref, b_ref, gain_ref, taps_ref, out_ref,
    scaled_ref, squares_ref, total_ref, glu_ref,
):
    step = pl.program_id(0)
    _, rows_in, width = x_ref.shape
    count, rows, channels = out_ref.shape
    half = channels // 2
    block = 32
    blocks = range(0, rows_in, block)

    @pl.when(step == 0)
    def _():
        squares_ref[...] = jnp.zeros_like(squares_ref)
        total_ref[...] = jnp.zeros_like(total_ref)

    for at in blocks:
        square = squares_ref[at : at + block]
        for b in range(0, width, 128):
            xf = x_ref[0, at : at + block, b : b + 128].astype(jnp.float32)
            square = square + xf * xf
            scaled = (xf * gain_ref[layer : layer + 1, b : b + 128]).astype(jnp.bfloat16)
            scaled_ref[at : at + block, b : b + 128] = scaled
        squares_ref[at : at + block] = square
    for k, w_ref in enumerate((a_ref, b_ref)):
        total_ref[k] += jnp.dot(scaled_ref[...], w_ref[0], preferred_element_type=jnp.float32)

    @pl.when(step == pl.num_programs(0) - 1)
    def _():
        swapped = order_ref[0] != 0
        for at in blocks:
            mean = jnp.sum(squares_ref[at : at + block], axis=1, keepdims=True)
            mean = mean / (pl.num_programs(0) * width)
            scale = lax.rsqrt(mean + 1e-06) * (1 / IN_SCALE)
            glu = []
            for k in range(2):
                value = total_ref[k, at : at + block, :half] * scale
                gate = total_ref[k, at : at + block, half:] * scale
                gated = (value * jax.nn.sigmoid(gate)).astype(jnp.bfloat16)
                glu.append(gated.astype(jnp.float32))
            glu_ref[0, at : at + block, :half] = jnp.where(swapped, glu[1], glu[0])
            glu_ref[0, at : at + block, half:] = jnp.where(swapped, glu[0], glu[1])
        reach_rows = rows_in - 8
        for shift in range(1, 8):
            glu_ref[shift, :reach_rows, :] = glu_ref[0, shift : shift + reach_rows, :]

        def convolve(i, carry):
            base = pl.multiple_of(i * block, block)
            for lane in range(0, channels, 128):
                lanes = slice(lane, lane + 128)
                conv = jnp.zeros((block, 128), jnp.float32)
                for tap in range(taps_ref.shape[0]):
                    down, shift = divmod(first + tap, 8)
                    moved = glu_ref[shift, pl.ds(pl.multiple_of(base + 8 * down, 8), block), lanes]
                    conv = conv + taps_ref[tap, layer : layer + 1, lanes] * moved
                conv = conv.astype(jnp.bfloat16)
                for c in range(count):
                    out_ref[c, pl.ds(base, block), lanes] = conv
            return carry

        lax.fori_loop(0, rows // block, convolve, 0)


def convolved(pieces, blocks, order, gains, taps, layer, rows):
    count, rows_in, width = pieces.shape
    taps = jnp.moveaxis(taps, 0, 1)
    channels = taps.shape[2]
    first = (rows_in - rows) // 2 - taps.shape[0] // 2
    blocks = [b.reshape(count, width, channels) for b in blocks]
    along = lambda *shape: pl.BlockSpec((1, *shape), lambda j: (j, 0, 0))
    return pl.pallas_call(
        functools.partial(convolved_kernel, first, layer),
        grid=(count,),
        out_shape=jax.ShapeDtypeStruct((count, rows, channels), jnp.bfloat16),
        in_specs=[
            pl.BlockSpec(memory_space=pltpu.SMEM),
            along(rows_in, width),
            along(width, channels),
            along(width, channels),
            pl.BlockSpec((gains.shape[0], width), lambda j: (0, j)),
            pl.BlockSpec(taps.shape, lambda j: (0, 0, 0)),
        ],
        out_specs=pl.BlockSpec((count, rows, channels), lambda j: (0, 0, 0)),
        scratch_shapes=[
            pltpu.VMEM((rows_in, width), jnp.bfloat16),
            pltpu.VMEM((rows_in, 128), jnp.float32),
            pltpu.VMEM((2, rows_in, channels), jnp.float32),
            pltpu.VMEM((8, rows_in, channels), jnp.float32),
        ],
        cost_estimate=pl.CostEstimate(
            flops=4 * rows_in * count * width * channels,
            bytes_accessed=4 * count * width * channels + 2 * count * rows_in * width,
            transcendentals=rows_in * channels,
        ),
    )(order.reshape(1), pieces, *blocks, gains, taps)


def activated(conv, gain):
    conv = conv.astype(jnp.float32)
    center = jnp.mean(conv, axis=1, keepdims=True)
    shifted = conv - center
    spread = jnp.mean(shifted * shifted, axis=1, keepdims=True)
    return jax.nn.silu(shifted * lax.rsqrt(spread + 1e-05) * gain[None, :]).astype(jnp.bfloat16)


def on_device(
    tokens, norm_gain, value_weight, gate_weight, conv_taps, channel_gain, out_weight, final_gain
):
    rows = tokens.shape[0]
    margin = 16
    groups = lax.axis_size("grp")
    paired = groups % 2 == 0
    order = lax.axis_index("grp") % 2 if paired else jnp.int32(0)
    swap = [(i, i ^ 1) for i in range(groups)]
    out_rows = out_weight.shape[1]
    sent, coded, slices = packed(
        value_weight, gate_weight, out_weight, channel_gain, order, paired
    )
    low, high = neighbours(tokens, "sp", 2 * margin)
    x_local = jnp.concatenate([low, tokens, high], axis=0)
    everyone = exchanged(jnp.concatenate([coded[:1], x_local[1:-1], coded[1:]], axis=0), "tp")
    x_local = x_local[margin:-margin]
    weights = lax.all_gather(sent.astype(jnp.float16), "sp")
    weights, everyone = lax.optimization_barrier((weights, everyone))

    def taken(at):
        return weights[:, at].astype(jnp.bfloat16)

    late_blocks = [taken(at) for at in slices[1][:-1]]
    if paired:
        late_blocks.append(lax.ppermute(late_blocks[0], "grp", swap))
    middle = rows + 2 * margin
    conv = convolved(
        everyone,
        [taken(at) for at in slices[0][:-1]],
        jnp.int32(0),
        norm_gain,
        conv_taps,
        0,
        middle,
    )
    conv, weights = lax.optimization_barrier((conv, weights))
    late_outs = [taken(slices[1][-1])]
    if paired:
        late_outs.append(lax.ppermute(late_outs[0], "grp", swap))
    conv_all = joined(lax.all_to_all(conv, "tp", 0, 0, tiled=True))
    gains = jnp.concatenate([everyone[:, 0], everyone[:, -1]], axis=1)[:, : 3 * channel_gain.size]
    gains = gains.reshape(-1, LAYERS, 3, channel_gain.shape[1]).astype(jnp.float32)
    gains = gains[:, :, 0] + (gains[:, :, 1] + gains[:, :, 2])
    gains = jnp.moveaxis(gains, 0, 1).reshape(LAYERS, -1)
    act = activated(conv_all, gains[0])
    branch = out_product(act, taken(slices[0][-1]), out_rows)
    position = lax.axis_index("sp") * rows - margin + lax.iota(jnp.int32, middle)
    inside = (position >= 0) & (position < rows * lax.axis_size("sp"))
    x_next = x_local.astype(jnp.float32) + branch
    x_next = jnp.where(inside[:, None], x_next, 0.0).astype(jnp.bfloat16)

    shared = (x_next.astype(jnp.float32) * X_SCALE).astype(jnp.float16)
    x_all = lax.all_gather(shared, "tp").astype(jnp.float32) * (1 / X_SCALE)
    conv = convolved(
        x_all.astype(jnp.bfloat16), late_blocks, order, norm_gain, conv_taps, 1, rows
    )
    conv_all = joined(lax.all_to_all(conv, "tp", 0, 0, tiled=True))
    act = activated(conv_all, gains[1])
    branches = [out_product(act, o, out_rows) for o in late_outs]
    if paired:
        own, other = branches
        branches = [jnp.where(order == 0, own, other), jnp.where(order == 0, other, own)]
    branch = jnp.concatenate(branches, axis=1)
    x_last = (x_next[margin : margin + rows].astype(jnp.float32) + branch).astype(jnp.bfloat16)

    xf = x_last.astype(jnp.float32)
    squares = jnp.sum(exchanged(jnp.sum(xf * xf, axis=1), "tp"), axis=0)
    width = xf.shape[1] * lax.axis_size("tp")
    scale = lax.rsqrt(squares / width + 1e-06)[:, None]
    return (xf * scale * final_gain[None, :]).astype(jnp.bfloat16)


def solution(mesh):
    placed = (
        P(("grp", "sp"), "tp"),
        P(),
        P(None, "sp", "tp"),
        P(None, "sp", "tp"),
        P(None, None, "tp"),
        P(None, "tp"),
        P(None, "sp", "tp"),
        P("tp"),
    )

    return jax.shard_map(
        on_device, mesh=mesh, in_specs=placed, out_specs=P(("grp", "sp"), "tp"), check_vma=False
    )
```

```python
import functools

import jax
import jax.numpy as jnp
from jax import lax
from jax.experimental import pallas as pl
from jax.experimental.pallas import tpu as pltpu
from jax.sharding import PartitionSpec as P


LAYERS = 2
IN_SCALE = 2.0**19
OUT_SCALE = 2.0**17
X_SCALE = 2.0**6


def exchanged(value, axis):
    size = lax.axis_size(axis)
    return lax.all_to_all(
        jnp.broadcast_to(value[None], (size, *value.shape)), axis, 0, 0, tiled=True
    )


def joined(pieces):
    size, rows, width = pieces.shape
    return jnp.moveaxis(pieces, 0, 1).reshape(rows, size * width)


def neighbours(block, axis, width):
    count = lax.axis_size(axis)
    forward = [(i, i + 1) for i in range(count - 1)]
    backward = [(i + 1, i) for i in range(count - 1)]
    low = lax.ppermute(block[block.shape[0] - width :], axis, forward)
    high = lax.ppermute(block[:width], axis, backward)
    return low, high


def packed_kernel(paired, order_ref, value_ref, gate_ref, out_ref, chan_ref, sent_ref, coded_ref):
    rows, channels = value_ref.shape[1:]
    out_rows, features = out_ref.shape[1:]
    half = channels // 2
    upper = order_ref[0] != 0
    at = 0

    def projection(layer, lower):
        lanes = slice(0, half) if lower else slice(half, channels)
        pair = value_ref[layer, :, lanes], gate_ref[layer, :, lanes]
        return [p.astype(jnp.float32) * IN_SCALE for p in pair]

    for layer in range(LAYERS):
        blocks = [projection(layer, True), projection(layer, False)]
        if paired and layer == LAYERS - 1:
            blocks = [[jnp.where(upper, high, low) for low, high in zip(*blocks)]]
        for value, gate in blocks:
            sent_ref[at : at + rows, :half] = value.astype(jnp.bfloat16)
            sent_ref[at : at + rows, half:] = gate.astype(jnp.bfloat16)
            at += rows
        starts = range(0, features, channels)
        blocks = [out_ref[layer, :, i : i + channels].astype(jnp.float32) * OUT_SCALE for i in starts]
        for block in blocks:
            sent_ref[at : at + out_rows] = block.astype(jnp.bfloat16)
            at += out_rows
    coded_ref[...] = jnp.zeros_like(coded_ref)
    for layer in range(LAYERS):
        rest = chan_ref[layer : layer + 1, :]
        for part in range(3):
            row, lane = divmod((layer * 3 + part) * channels, coded_ref.shape[1])
            coded = rest.astype(jnp.bfloat16)
            coded_ref[row : row + 1, lane : lane + channels] = coded
            rest = rest - coded.astype(jnp.float32)


def packed(value, gate, out, chan_gain, order, paired):
    rows, channels = value.shape[1:]
    out_rows, features = out.shape[1:]
    slices, at = [], 0
    for layer in range(LAYERS):
        of_layer = []
        for _ in range(1 if paired and layer == LAYERS - 1 else 2):
            of_layer.append(slice(at, at + rows))
            at += rows
        of_layer.append(slice(at, at + out_rows * (features // channels)))
        at = of_layer[-1].stop
        slices.append(of_layer)
    vmem = pl.BlockSpec(memory_space=pltpu.VMEM)
    sent, coded = pl.pallas_call(
        functools.partial(packed_kernel, paired),
        out_shape=(
            jax.ShapeDtypeStruct((at, channels), jnp.bfloat16),
            jax.ShapeDtypeStruct((2, features), jnp.bfloat16),
        ),
        in_specs=[pl.BlockSpec(memory_space=pltpu.SMEM), vmem, vmem, vmem, vmem],
        out_specs=(vmem, vmem),
    )(order.reshape(1), value, gate, out, chan_gain)
    return sent, coded, slices


def out_product(act, block, rows):
    parts, height, width = block.shape
    return jnp.concatenate(
        [
            jnp.dot(
                act,
                block[:, i : i + rows].reshape(parts * rows, width),
                preferred_element_type=jnp.float32,
            )
            for i in range(0, height, rows)
        ],
        axis=1,
    ) * (1 / OUT_SCALE)


def convolved_kernel(
    first, layer, order_ref, x_ref, a_ref, b_ref, gain_ref, taps_ref, out_ref,
    scaled_ref, squares_ref, total_ref, glu_ref,
):
    step = pl.program_id(0)
    _, rows_in, width = x_ref.shape
    count, rows, channels = out_ref.shape
    half = channels // 2
    block = 32
    blocks = range(0, rows_in, block)

    @pl.when(step == 0)
    def _():
        squares_ref[...] = jnp.zeros_like(squares_ref)
        total_ref[...] = jnp.zeros_like(total_ref)

    for at in blocks:
        square = squares_ref[at : at + block]
        for b in range(0, width, 128):
            xf = x_ref[0, at : at + block, b : b + 128].astype(jnp.float32)
            square = square + xf * xf
            scaled = (xf * gain_ref[layer : layer + 1, b : b + 128]).astype(jnp.bfloat16)
            scaled_ref[at : at + block, b : b + 128] = scaled
        squares_ref[at : at + block] = square
    for k, w_ref in enumerate((a_ref, b_ref)):
        total_ref[k] += jnp.dot(scaled_ref[...], w_ref[0], preferred_element_type=jnp.float32)

    @pl.when(step == pl.num_programs(0) - 1)
    def _():
        swapped = order_ref[0] != 0
        for at in blocks:
            mean = jnp.sum(squares_ref[at : at + block], axis=1, keepdims=True)
            mean = mean / (pl.num_programs(0) * width)
            scale = lax.rsqrt(mean + 1e-06) * (1 / IN_SCALE)
            glu = []
            for k in range(2):
                value = total_ref[k, at : at + block, :half] * scale
                gate = total_ref[k, at : at + block, half:] * scale
                gated = (value * jax.nn.sigmoid(gate)).astype(jnp.bfloat16)
                glu.append(gated.astype(jnp.float32))
            glu_ref[0, at : at + block, :half] = jnp.where(swapped, glu[1], glu[0])
            glu_ref[0, at : at + block, half:] = jnp.where(swapped, glu[0], glu[1])
        reach_rows = rows_in - 8
        for shift in range(1, 8):
            glu_ref[shift, :reach_rows, :] = glu_ref[0, shift : shift + reach_rows, :]

        def convolve(i, carry):
            base = pl.multiple_of(i * block, block)
            for lane in range(0, channels, 128):
                lanes = slice(lane, lane + 128)
                conv = jnp.zeros((block, 128), jnp.float32)
                for tap in range(taps_ref.shape[0]):
                    down, shift = divmod(first + tap, 8)
                    moved = glu_ref[shift, pl.ds(pl.multiple_of(base + 8 * down, 8), block), lanes]
                    conv = conv + taps_ref[tap, layer : layer + 1, lanes] * moved
                conv = conv.astype(jnp.bfloat16)
                for c in range(count):
                    out_ref[c, pl.ds(base, block), lanes] = conv
            return carry

        lax.fori_loop(0, rows // block, convolve, 0)


def convolved(pieces, blocks, order, gains, taps, layer, rows):
    count, rows_in, width = pieces.shape
    taps = jnp.moveaxis(taps, 0, 1)
    channels = taps.shape[2]
    first = (rows_in - rows) // 2 - taps.shape[0] // 2
    blocks = [b.reshape(count, width, channels) for b in blocks]
    along = lambda *shape: pl.BlockSpec((1, *shape), lambda j: (j, 0, 0))
    return pl.pallas_call(
        functools.partial(convolved_kernel, first, layer),
        grid=(count,),
        out_shape=jax.ShapeDtypeStruct((count, rows, channels), jnp.bfloat16),
        in_specs=[
            pl.BlockSpec(memory_space=pltpu.SMEM),
            along(rows_in, width),
            along(width, channels),
            along(width, channels),
            pl.BlockSpec((gains.shape[0], width), lambda j: (0, j)),
            pl.BlockSpec(taps.shape, lambda j: (0, 0, 0)),
        ],
        out_specs=pl.BlockSpec((count, rows, channels), lambda j: (0, 0, 0)),
        scratch_shapes=[
            pltpu.VMEM((rows_in, width), jnp.bfloat16),
            pltpu.VMEM((rows_in, 128), jnp.float32),
            pltpu.VMEM((2, rows_in, channels), jnp.float32),
            pltpu.VMEM((8, rows_in, channels), jnp.float32),
        ],
        cost_estimate=pl.CostEstimate(
            flops=4 * rows_in * count * width * channels,
            bytes_accessed=4 * count * width * channels + 2 * count * rows_in * width,
            transcendentals=rows_in * channels,
        ),
    )(order.reshape(1), pieces, *blocks, gains, taps)


def activated(conv, gain):
    conv = conv.astype(jnp.float32)
    center = jnp.mean(conv, axis=1, keepdims=True)
    shifted = conv - center
    spread = jnp.mean(shifted * shifted, axis=1, keepdims=True)
    return jax.nn.silu(shifted * lax.rsqrt(spread + 1e-05) * gain[None, :]).astype(jnp.bfloat16)


def on_device(
    tokens, norm_gain, value_weight, gate_weight, conv_taps, channel_gain, out_weight, final_gain
):
    rows = tokens.shape[0]
    margin = 16
    groups = lax.axis_size("grp")
    paired = groups % 2 == 0
    order = lax.axis_index("grp") % 2 if paired else jnp.int32(0)
    swap = [(i, i ^ 1) for i in range(groups)]
    out_rows = out_weight.shape[1]
    sent, coded, slices = packed(
        value_weight, gate_weight, out_weight, channel_gain, order, paired
    )
    low, high = neighbours(tokens, "sp", 2 * margin)
    x_local = jnp.concatenate([low, tokens, high], axis=0)
    everyone = exchanged(jnp.concatenate([coded[:1], x_local[1:-1], coded[1:]], axis=0), "tp")
    x_local = x_local[margin:-margin]
    weights = lax.all_gather(sent.astype(jnp.float16), "sp")

    def taken(at):
        return weights[:, at].astype(jnp.bfloat16)

    late_blocks = [taken(at) for at in slices[1][:-1]]
    if paired:
        late_blocks.append(lax.ppermute(late_blocks[0], "grp", swap))
    middle = rows + 2 * margin
    conv = convolved(
        everyone,
        [taken(at) for at in slices[0][:-1]],
        jnp.int32(0),
        norm_gain,
        conv_taps,
        0,
        middle,
    )
    conv, weights = lax.optimization_barrier((conv, weights))
    conv_all = joined(lax.all_to_all(conv, "tp", 0, 0, tiled=True))
    gains = jnp.concatenate([everyone[:, 0], everyone[:, -1]], axis=1)[:, : 3 * channel_gain.size]
    gains = gains.reshape(-1, LAYERS, 3, channel_gain.shape[1]).astype(jnp.float32)
    gains = gains[:, :, 0] + (gains[:, :, 1] + gains[:, :, 2])
    gains = jnp.moveaxis(gains, 0, 1).reshape(LAYERS, -1)
    act = activated(conv_all, gains[0])
    branch = out_product(act, taken(slices[0][-1]), out_rows)
    position = lax.axis_index("sp") * rows - margin + lax.iota(jnp.int32, middle)
    inside = (position >= 0) & (position < rows * lax.axis_size("sp"))
    x_next = x_local.astype(jnp.float32) + branch
    x_next = jnp.where(inside[:, None], x_next, 0.0).astype(jnp.bfloat16)

    shared = (x_next.astype(jnp.float32) * X_SCALE).astype(jnp.float16)
    x_all = lax.all_gather(shared, "tp").astype(jnp.float32) * (1 / X_SCALE)
    conv = convolved(
        x_all.astype(jnp.bfloat16), late_blocks, order, norm_gain, conv_taps, 1, rows
    )
    conv, weights = lax.optimization_barrier((conv, weights))
    conv_all = joined(lax.all_to_all(conv, "tp", 0, 0, tiled=True))
    act = activated(conv_all, gains[1])
    branch = out_product(act, taken(slices[1][-1]), out_rows)
    x_last = (x_next[margin : margin + rows].astype(jnp.float32) + branch).astype(jnp.bfloat16)

    xf = x_last.astype(jnp.float32)
    squares = jnp.sum(exchanged(jnp.sum(xf * xf, axis=1), "tp"), axis=0)
    width = xf.shape[1] * lax.axis_size("tp")
    scale = lax.rsqrt(squares / width + 1e-06)[:, None]
    return (xf * scale * final_gain[None, :]).astype(jnp.bfloat16)


def solution(mesh):
    placed = (
        P(("grp", "sp"), "tp"),
        P(),
        P(None, "sp", "tp"),
        P(None, "sp", "tp"),
        P(None, None, "tp"),
        P(None, "tp"),
        P(None, "sp", "tp"),
        P("tp"),
    )

    return jax.shard_map(
        on_device, mesh=mesh, in_specs=placed, out_specs=P(("grp", "sp"), "tp"), check_vma=False
    )
```

```python
import functools

import jax
import jax.numpy as jnp
from jax import lax
from jax.experimental import pallas as pl
from jax.experimental.pallas import tpu as pltpu
from jax.sharding import PartitionSpec as P


LAYERS = 2
IN_SCALE = 2.0**19
OUT_SCALE = 2.0**17
X_SCALE = 2.0**6


def exchanged(value, axis):
    size = lax.axis_size(axis)
    return lax.all_to_all(
        jnp.broadcast_to(value[None], (size, *value.shape)), axis, 0, 0, tiled=True
    )


def joined(pieces):
    size, rows, width = pieces.shape
    return jnp.moveaxis(pieces, 0, 1).reshape(rows, size * width)


def neighbours(block, axis, width):
    count = lax.axis_size(axis)
    forward = [(i, i + 1) for i in range(count - 1)]
    backward = [(i + 1, i) for i in range(count - 1)]
    low = lax.ppermute(block[block.shape[0] - width :], axis, forward)
    high = lax.ppermute(block[:width], axis, backward)
    return low, high


def packed_kernel(paired, order_ref, value_ref, gate_ref, out_ref, chan_ref, sent_ref, coded_ref):
    rows, channels = value_ref.shape[1:]
    out_rows, features = out_ref.shape[1:]
    half = channels // 2
    upper = order_ref[0] != 0
    at = 0

    def projection(layer, lower):
        lanes = slice(0, half) if lower else slice(half, channels)
        pair = value_ref[layer, :, lanes], gate_ref[layer, :, lanes]
        return [p.astype(jnp.float32) * IN_SCALE for p in pair]

    for layer in range(LAYERS):
        blocks = [projection(layer, True), projection(layer, False)]
        if paired and layer == LAYERS - 1:
            blocks = [[jnp.where(upper, high, low) for low, high in zip(*blocks)]]
        for value, gate in blocks:
            sent_ref[at : at + rows, :half] = value.astype(jnp.bfloat16)
            sent_ref[at : at + rows, half:] = gate.astype(jnp.bfloat16)
            at += rows
        starts = range(0, features, channels)
        blocks = [out_ref[layer, :, i : i + channels].astype(jnp.float32) * OUT_SCALE for i in starts]
        if paired and layer == LAYERS - 1:
            blocks = [*blocks[:-2], jnp.where(upper, blocks[-1], blocks[-2])]
        for block in blocks:
            sent_ref[at : at + out_rows] = block.astype(jnp.bfloat16)
            at += out_rows
    coded_ref[...] = jnp.zeros_like(coded_ref)
    for layer in range(LAYERS):
        rest = chan_ref[layer : layer + 1, :]
        for part in range(3):
            row, lane = divmod((layer * 3 + part) * channels, coded_ref.shape[1])
            coded = rest.astype(jnp.bfloat16)
            coded_ref[row : row + 1, lane : lane + channels] = coded
            rest = rest - coded.astype(jnp.float32)


def packed(value, gate, out, chan_gain, order, paired):
    rows, channels = value.shape[1:]
    out_rows, features = out.shape[1:]
    slices, at = [], 0
    for layer in range(LAYERS):
        of_layer = []
        for _ in range(1 if paired and layer == LAYERS - 1 else 2):
            of_layer.append(slice(at, at + rows))
            at += rows
        spared = 1 if paired and layer == LAYERS - 1 else 0
        of_layer.append(slice(at, at + out_rows * (features // channels - spared)))
        at = of_layer[-1].stop
        slices.append(of_layer)
    vmem = pl.BlockSpec(memory_space=pltpu.VMEM)
    sent, coded = pl.pallas_call(
        functools.partial(packed_kernel, paired),
        out_shape=(
            jax.ShapeDtypeStruct((at, channels), jnp.bfloat16),
            jax.ShapeDtypeStruct((2, features), jnp.bfloat16),
        ),
        in_specs=[pl.BlockSpec(memory_space=pltpu.SMEM), vmem, vmem, vmem, vmem],
        out_specs=(vmem, vmem),
    )(order.reshape(1), value, gate, out, chan_gain)
    return sent, coded, slices


def out_product(act, block, rows):
    parts, height, width = block.shape
    return jnp.concatenate(
        [
            jnp.dot(
                act,
                block[:, i : i + rows].reshape(parts * rows, width),
                preferred_element_type=jnp.float32,
            )
            for i in range(0, height, rows)
        ],
        axis=1,
    ) * (1 / OUT_SCALE)


def convolved_kernel(
    first, layer, order_ref, x_ref, a_ref, b_ref, gain_ref, taps_ref, out_ref,
    scaled_ref, squares_ref, total_ref, glu_ref,
):
    step = pl.program_id(0)
    _, rows_in, width = x_ref.shape
    count, rows, channels = out_ref.shape
    half = channels // 2
    block = 32
    blocks = range(0, rows_in, block)

    @pl.when(step == 0)
    def _():
        squares_ref[...] = jnp.zeros_like(squares_ref)
        total_ref[...] = jnp.zeros_like(total_ref)

    for at in blocks:
        square = squares_ref[at : at + block]
        for b in range(0, width, 128):
            xf = x_ref[0, at : at + block, b : b + 128].astype(jnp.float32)
            square = square + xf * xf
            scaled = (xf * gain_ref[layer : layer + 1, b : b + 128]).astype(jnp.bfloat16)
            scaled_ref[at : at + block, b : b + 128] = scaled
        squares_ref[at : at + block] = square
    for k, w_ref in enumerate((a_ref, b_ref)):
        total_ref[k] += jnp.dot(scaled_ref[...], w_ref[0], preferred_element_type=jnp.float32)

    @pl.when(step == pl.num_programs(0) - 1)
    def _():
        swapped = order_ref[0] != 0
        for at in blocks:
            mean = jnp.sum(squares_ref[at : at + block], axis=1, keepdims=True)
            mean = mean / (pl.num_programs(0) * width)
            scale = lax.rsqrt(mean + 1e-06) * (1 / IN_SCALE)
            glu = []
            for k in range(2):
                value = total_ref[k, at : at + block, :half] * scale
                gate = total_ref[k, at : at + block, half:] * scale
                gated = (value * jax.nn.sigmoid(gate)).astype(jnp.bfloat16)
                glu.append(gated.astype(jnp.float32))
            glu_ref[0, at : at + block, :half] = jnp.where(swapped, glu[1], glu[0])
            glu_ref[0, at : at + block, half:] = jnp.where(swapped, glu[0], glu[1])
        reach_rows = rows_in - 8
        for shift in range(1, 8):
            glu_ref[shift, :reach_rows, :] = glu_ref[0, shift : shift + reach_rows, :]

        def convolve(i, carry):
            base = pl.multiple_of(i * block, block)
            for lane in range(0, channels, 128):
                lanes = slice(lane, lane + 128)
                conv = jnp.zeros((block, 128), jnp.float32)
                for tap in range(taps_ref.shape[0]):
                    down, shift = divmod(first + tap, 8)
                    moved = glu_ref[shift, pl.ds(pl.multiple_of(base + 8 * down, 8), block), lanes]
                    conv = conv + taps_ref[tap, layer : layer + 1, lanes] * moved
                conv = conv.astype(jnp.bfloat16)
                for c in range(count):
                    out_ref[c, pl.ds(base, block), lanes] = conv
            return carry

        lax.fori_loop(0, rows // block, convolve, 0)


def convolved(pieces, blocks, order, gains, taps, layer, rows):
    count, rows_in, width = pieces.shape
    taps = jnp.moveaxis(taps, 0, 1)
    channels = taps.shape[2]
    first = (rows_in - rows) // 2 - taps.shape[0] // 2
    blocks = [b.reshape(count, width, channels) for b in blocks]
    along = lambda *shape: pl.BlockSpec((1, *shape), lambda j: (j, 0, 0))
    return pl.pallas_call(
        functools.partial(convolved_kernel, first, layer),
        grid=(count,),
        out_shape=jax.ShapeDtypeStruct((count, rows, channels), jnp.bfloat16),
        in_specs=[
            pl.BlockSpec(memory_space=pltpu.SMEM),
            along(rows_in, width),
            along(width, channels),
            along(width, channels),
            pl.BlockSpec((gains.shape[0], width), lambda j: (0, j)),
            pl.BlockSpec(taps.shape, lambda j: (0, 0, 0)),
        ],
        out_specs=pl.BlockSpec((count, rows, channels), lambda j: (0, 0, 0)),
        scratch_shapes=[
            pltpu.VMEM((rows_in, width), jnp.bfloat16),
            pltpu.VMEM((rows_in, 128), jnp.float32),
            pltpu.VMEM((2, rows_in, channels), jnp.float32),
            pltpu.VMEM((8, rows_in, channels), jnp.float32),
        ],
        cost_estimate=pl.CostEstimate(
            flops=4 * rows_in * count * width * channels,
            bytes_accessed=4 * count * width * channels + 2 * count * rows_in * width,
            transcendentals=rows_in * channels,
        ),
    )(order.reshape(1), pieces, *blocks, gains, taps)


def activated(conv, gain):
    conv = conv.astype(jnp.float32)
    center = jnp.mean(conv, axis=1, keepdims=True)
    shifted = conv - center
    spread = jnp.mean(shifted * shifted, axis=1, keepdims=True)
    return jax.nn.silu(shifted * lax.rsqrt(spread + 1e-05) * gain[None, :]).astype(jnp.bfloat16)


def on_device(
    tokens, norm_gain, value_weight, gate_weight, conv_taps, channel_gain, out_weight, final_gain
):
    rows = tokens.shape[0]
    margin = 16
    groups = lax.axis_size("grp")
    paired = groups % 2 == 0
    order = lax.axis_index("grp") % 2 if paired else jnp.int32(0)
    swap = [(i, i ^ 1) for i in range(groups)]
    out_rows = out_weight.shape[1]
    sent, coded, slices = packed(
        value_weight, gate_weight, out_weight, channel_gain, order, paired
    )
    low, high = neighbours(tokens, "sp", 2 * margin)
    x_local = jnp.concatenate([low, tokens, high], axis=0)
    everyone = exchanged(jnp.concatenate([coded[:1], x_local[1:-1], coded[1:]], axis=0), "tp")
    x_local = x_local[margin:-margin]
    weights = lax.all_gather(sent.astype(jnp.float16), "sp")

    def taken(at):
        return weights[:, at].astype(jnp.bfloat16)

    late_blocks = [taken(at) for at in slices[1][:-1]]
    if paired:
        late_blocks.append(lax.ppermute(late_blocks[0], "grp", swap))
    middle = rows + 2 * margin
    conv = convolved(
        everyone,
        [taken(at) for at in slices[0][:-1]],
        jnp.int32(0),
        norm_gain,
        conv_taps,
        0,
        middle,
    )
    conv, weights = lax.optimization_barrier((conv, weights))
    late_out = slices[1][-1]
    if paired:
        late_out = slice(late_out.start, late_out.stop - out_rows)
        own_out = taken(slice(late_out.stop, late_out.stop + out_rows))
        other_out = lax.ppermute(own_out, "grp", swap)
    conv_all = joined(lax.all_to_all(conv, "tp", 0, 0, tiled=True))
    gains = jnp.concatenate([everyone[:, 0], everyone[:, -1]], axis=1)[:, : 3 * channel_gain.size]
    gains = gains.reshape(-1, LAYERS, 3, channel_gain.shape[1]).astype(jnp.float32)
    gains = gains[:, :, 0] + (gains[:, :, 1] + gains[:, :, 2])
    gains = jnp.moveaxis(gains, 0, 1).reshape(LAYERS, -1)
    act = activated(conv_all, gains[0])
    branch = out_product(act, taken(slices[0][-1]), out_rows)
    position = lax.axis_index("sp") * rows - margin + lax.iota(jnp.int32, middle)
    inside = (position >= 0) & (position < rows * lax.axis_size("sp"))
    x_next = x_local.astype(jnp.float32) + branch
    x_next = jnp.where(inside[:, None], x_next, 0.0).astype(jnp.bfloat16)

    shared = (x_next.astype(jnp.float32) * X_SCALE).astype(jnp.float16)
    x_all = lax.all_gather(shared, "tp").astype(jnp.float32) * (1 / X_SCALE)
    conv = convolved(
        x_all.astype(jnp.bfloat16), late_blocks, order, norm_gain, conv_taps, 1, rows
    )
    conv, weights = lax.optimization_barrier((conv, weights))
    conv_all = joined(lax.all_to_all(conv, "tp", 0, 0, tiled=True))
    act = activated(conv_all, gains[1])
    branch = out_product(act, taken(late_out), out_rows)
    if paired:
        own, other = [out_product(act, o, out_rows) for o in (own_out, other_out)]
        last_two = jnp.where(order == 0, own, other), jnp.where(order == 0, other, own)
        branch = jnp.concatenate([branch, *last_two], axis=1)
    x_last = (x_next[margin : margin + rows].astype(jnp.float32) + branch).astype(jnp.bfloat16)

    xf = x_last.astype(jnp.float32)
    squares = jnp.sum(exchanged(jnp.sum(xf * xf, axis=1), "tp"), axis=0)
    width = xf.shape[1] * lax.axis_size("tp")
    scale = lax.rsqrt(squares / width + 1e-06)[:, None]
    return (xf * scale * final_gain[None, :]).astype(jnp.bfloat16)


def solution(mesh):
    placed = (
        P(("grp", "sp"), "tp"),
        P(),
        P(None, "sp", "tp"),
        P(None, "sp", "tp"),
        P(None, None, "tp"),
        P(None, "tp"),
        P(None, "sp", "tp"),
        P("tp"),
    )

    return jax.shard_map(
        on_device, mesh=mesh, in_specs=placed, out_specs=P(("grp", "sp"), "tp"), check_vma=False
    )
```
